32 devices in a mesh: sp: 8 (over z, y), dp: 4 (over x, core).
Axes of the slice: x: 2, y: 2, z: 4, core: 2. Of those that a mesh axis runs over, the one named last changes fastest.
Arguments:
- skip_connection_stream: bfloat16 [4, 1024, 2048], P('dp', 'sp'), may hold values from -6 to 6
- emitted_valve_unscaled: bfloat16 [4, 1024, 1024], P('dp', 'sp'), may hold values from -6 to 6
- channel_source_mapped: bfloat16 [4, 1024, 1024], P('dp', 'sp'), may hold values from -6 to 6
- hidden_source_mapped: bfloat16 [4, 1024, 256], P('dp', 'sp'), may hold values from -6 to 6
- probe_mapped_values: bfloat16 [4, 1024, 256], P('dp', 'sp'), may hold values from -6 to 6
- increment_premapped: float32 [4, 1024, 16], P('dp', None, 'sp'), may hold values from -6 to 6
- extra_log_fading: float32 [4, 1024, 16], P('dp', None, 'sp'), may hold values from -2 to 0
- channel_fading_speed: float32 [16], replicated, may hold values from 0 to 1, as said below
- channel_source_kernel: float32 [4, 1024], replicated, may hold values from -3 to 3
- hidden_source_kernel: float32 [4, 256], replicated, may hold values from -3 to 3
- probe_kernel_coefficients: float32 [4, 256], replicated, may hold values from -3 to 3
- cluster_scaling_factor: float32 [1024], replicated, may hold values from 0.1 to 1.9
- emitted_mapping_matrix: bfloat16 [1024, 2048], replicated, may hold values from -0.1875 to 0.1875
- standardize_scaling: float32 [2048], replicated, may hold values from 0.1 to 1.9
- standardize_offset: float32 [2048], replicated, may hold values from -2 to 2
- chosen_specialist_ids: int32 [4, 1024, 2], P('dp', 'sp'), may hold values from 0 to 7, all different within a row; in each aligned block of 128 rows (0 to 127, 128 to 255, ..., all dimensions but the last counted through in order) at most 48 rows name the same one
- specialist_mixing_shares: float32 [4, 1024, 2], P('dp', 'sp'), may hold values from 0.2 to 1
- specialist_gating_matrices: bfloat16 [8, 2048, 5120], P('sp', None, 'dp'), may hold values from -0.125 to 0.125
- raising_matrices: bfloat16 [8, 2048, 5120], P('sp', None, 'dp'), may hold values from -0.125 to 0.125
- lowering_matrices: bfloat16 [8, 5120, 2048], P('sp', 'dp'), may hold values from -0.078125 to 0.078125
Outputs:
- layer_out: bfloat16 [4, 1024, 2048], P('dp', 'sp')
The draws below stay inside these ranges and needn't reach their ends.
Inputs may be any that keep to these rules, and one draw needn't show every extreme that they name: `chosen_specialist_ids`: each row names two different experts. The rows of one device name no expert more than 48 times, a bound that some block reaches. `channel_fading_speed`: Positive.
All inputs are finite; a program needn't handle non-finite values.
Results may differ from the reference program's by a relative error of at most 0.015.
Values may be sent and summed in bfloat16 or wider, within the bound.
No kernel may reach another device: no remote copies, remote signals or barrier semaphores. Data moves between devices by JAX's collectives and lax.ppermute only.
A program may use at most 128 MiB of HBM per device.

```python
import math
import jax
import jax.numpy as jnp
import numpy as np
from jax import lax

D = 2048
HEADS = 16
HEAD_DIM = 64
GROUPS = 4
STATE = 64
FF = 5120
KERNEL = 4
BLK = 128
TOK = 128
INNER = 1024
EXPERTS = 8
CAP = 48
FF_PART = 1280
LEN = 1024
BATCH = 4
N_SP = 8
N_DP = 4


def draw_increment_premapped(key, part):
    noise_key, shift_key = jax.random.split(key)
    block_count = LEN // TOK
    shifted = jax.random.uniform(shift_key, (BATCH, block_count, 1, HEADS), jnp.float32, -1.2, 1.2)
    noise = jax.random.normal(noise_key, (BATCH, block_count, TOK, HEADS), jnp.float32)
    return jnp.clip(noise + shifted, -6.0, 6.0).reshape(BATCH, LEN, HEADS)


def draw_extra_log_fading(key, part):
    spot_key, loss_key = jax.random.split(key)
    spots = jax.random.randint(spot_key, (BATCH, 1, HEADS, 2), 0, LEN)
    losses = jax.random.uniform(loss_key, (BATCH, 1, HEADS, 2), jnp.float32, 0.2, 0.5)
    matched = jnp.arange(LEN)[None, :, None, None] == spots
    return jnp.sum(jnp.where(matched, jnp.log(1.0 - losses), 0.0), axis=3)


def draw_channel_fading_speed(key, part):
    pick_key, fast_key, slow_key = jax.random.split(key, 3)
    fast_share = 0.5
    quick = jax.random.bernoulli(pick_key, fast_share, (HEADS,))
    fast_rate = jnp.exp(jax.random.uniform(fast_key, (HEADS,), jnp.float32, math.log(0.03), math.log(0.1))) / 0.8
    slow_rate = jnp.exp(jax.random.uniform(slow_key, (HEADS,), jnp.float32, math.log(0.2), math.log(0.8))) / (0.8 * LEN)
    return jnp.where(quick, fast_rate, slow_rate)


def block_scale(rng, extent, cuts, least, high):
    def one(dim, blocks):
        heights = jax.random.uniform(jax.random.fold_in(jax.random.fold_in(rng, 6), dim), (blocks,), jnp.float32, least / len(cuts), high / len(cuts))
        return jnp.repeat(jnp.exp(heights), extent[dim] // blocks).reshape((-1,) + (1,) * (len(extent) - dim - 1))

    gain = one(*cuts[0])
    for cut in cuts[1:]:
        gain = gain * one(*cut)
    return gain


def deal_out(stream_key, own, number, rows, number_of, top, reach, skew):
    sequence = jax.random.permutation(stream_key, number_of)
    crowded, common = portions_of(number_of, rows * top, reach, skew, True), portions_of(number_of, rows * top, reach, skew, False)
    places = jnp.arange(number_of)

    def named(lengths, rotation):
        used = int((lengths > 0).sum())
        fixed = max(1, used // 4)
        passed = fixed + (places - fixed + rotation * (used - fixed)) % max(1, number_of - fixed)
        return jnp.zeros((number_of,), jnp.int32).at[sequence[jnp.where(places < fixed, places, passed)]].set(jnp.asarray(lengths, jnp.int32))

    lengths = jnp.where(number % 4 == 0, named(crowded, number // 4), named(common, number - number // 4 - 1))
    mixed = jax.random.permutation(jax.random.fold_in(own, 3), number_of)
    donor, taker = mixed[0:number_of // 2 * 2:2], mixed[1:number_of // 2 * 2:2]
    room = jnp.minimum(lengths[donor] - 1, reach - lengths[taker]) // 2
    room = jnp.where((donor == sequence[0]) | (taker == sequence[0]) | (lengths[taker] == 0), 0, jnp.maximum(room, 0))
    passed = jax.random.randint(jax.random.fold_in(own, 4), (number_of // 2,), 0, 1 << 20) % (room + 1)
    lengths = lengths.at[donor].add(-passed).at[taker].add(passed)
    members = jnp.searchsorted(jnp.cumsum(lengths), jnp.arange(rows * top), side="right").astype(jnp.int32)
    grid = members.reshape(top, rows).T
    grid = grid[jax.random.permutation(jax.random.fold_in(own, 1), rows)]
    rotation = jax.random.randint(jax.random.fold_in(own, 2), (rows, 1), 0, top)
    return jnp.take_along_axis(grid, (jnp.arange(top)[None, :] + rotation) % top, axis=1)


def portions_of(amount, total, limit, lean, full):
    loads = [(1 << 20) // math.isqrt(grade ** lean) + 1 for grade in range(1, amount + 1)]
    largest = limit if full else min(limit, max(-(-total // amount), total * loads[0] // sum(loads)))
    least = 1 if total - largest >= amount - 1 else 0
    given, rest = [largest] + [least] * (amount - 1), total - largest - least * (amount - 1)
    while rest > 0:
        free = [i for i in range(1, amount) if given[i] < largest] or [i for i in range(1, amount) if given[i] < limit]
        whole, left = sum([loads[i] for i in free]), rest
        for i in free:
            more = min(limit - given[i], max(1, left * loads[i] // whole), rest)
            given[i] = given[i] + more
            rest = rest - more
    return np.array(given)


def bell_draw(rng, dims, scale, limit, cuts=(), held_as=jnp.bfloat16):
    array = scale * jax.random.normal(rng, dims, jnp.float32)
    if cuts:
        array = array * block_scale(rng, dims, cuts, -0.22, 0.18)
    return jnp.clip(array, -limit, limit).astype(held_as)


def setup_inputs(seed: int = 0) -> dict:
    key_list = jax.random.split(jax.random.key(seed), 21)
    skip_connection_stream = bell_draw(key_list[0], (BATCH, LEN, D), 1.0, 6.0, ((0, 4), (1, 8)))
    emitted_valve_unscaled = bell_draw(key_list[1], (BATCH, LEN, INNER), 1.0, 6.0, ((0, 4), (1, 8)))
    channel_source_mapped = bell_draw(key_list[2], (BATCH, LEN, INNER), 1.0, 6.0, ((0, 4), (1, 8)))
    hidden_source_mapped = bell_draw(key_list[3], (BATCH, LEN, GROUPS * STATE), 1.0, 6.0, ((0, 4), (1, 8)))
    probe_mapped_values = bell_draw(key_list[4], (BATCH, LEN, GROUPS * STATE), 1.0, 6.0, ((0, 4), (1, 8)))
    increment_premapped = draw_increment_premapped(jax.random.fold_in(key_list[20], 71), 0)
    extra_log_fading = draw_extra_log_fading(jax.random.fold_in(key_list[20], 71), 0)
    channel_fading_speed = draw_channel_fading_speed(jax.random.fold_in(key_list[20], 71), 0)
    channel_source_kernel = bell_draw(key_list[8], (KERNEL, INNER), KERNEL ** -0.5, 3.0, (), jnp.float32)
    hidden_source_kernel = bell_draw(key_list[9], (KERNEL, GROUPS * STATE), KERNEL ** -0.5, 3.0, (), jnp.float32)
    probe_kernel_coefficients = bell_draw(key_list[10], (KERNEL, GROUPS * STATE), KERNEL ** -0.5, 3.0, (), jnp.float32)
    cluster_scaling_factor = jnp.clip(1.0 + 0.18 * jax.random.normal(key_list[11], (INNER,), jnp.float32), 0.1, 1.9)
    emitted_mapping_matrix = bell_draw(key_list[12], (INNER, D), INNER ** -0.5, 0.1875)
    standardize_scaling = jnp.clip(1.0 + 0.18 * jax.random.normal(key_list[13], (D,), jnp.float32), 0.1, 1.9)
    standardize_offset = bell_draw(key_list[14], (D,), 0.3, 2.0, (), jnp.float32)
    chosen_specialist_ids_keys = jax.random.split(jax.random.fold_in(key_list[15], 1), BATCH * LEN // TOK)
    chosen_specialist_ids_turns = jax.random.permutation(jax.random.fold_in(key_list[15], 3), BATCH * LEN // TOK)
    chosen_specialist_ids = jax.vmap(lambda own, number: deal_out(jax.random.fold_in(key_list[15], 2), own, number, TOK, EXPERTS, 2, CAP, 2))(chosen_specialist_ids_keys, chosen_specialist_ids_turns).reshape((BATCH, LEN, 2))
    specialist_mixing_shares = jnp.clip(0.2 + 0.8 * jax.random.uniform(key_list[16], (BATCH, LEN, 2), jnp.float32) ** block_scale(key_list[16], (BATCH, LEN, 2), ((0, 4), (1, 8)), -0.2, 0.2), 0.2, 1.0)
    specialist_gating_matrices = bell_draw(key_list[17], (EXPERTS, D, FF), D ** -0.5, 0.125, ((0, 8), (2, 4)))
    raising_matrices = bell_draw(key_list[18], (EXPERTS, D, FF), D ** -0.5, 0.125, ((0, 8), (2, 4)))
    lowering_matrices = bell_draw(key_list[19], (EXPERTS, FF, D), FF ** -0.5, 0.078125, ((0, 8), (1, 4)))
    return dict(skip_connection_stream=skip_connection_stream, emitted_valve_unscaled=emitted_valve_unscaled, channel_source_mapped=channel_source_mapped, hidden_source_mapped=hidden_source_mapped, probe_mapped_values=probe_mapped_values, increment_premapped=increment_premapped, extra_log_fading=extra_log_fading, channel_fading_speed=channel_fading_speed, channel_source_kernel=channel_source_kernel, hidden_source_kernel=hidden_source_kernel, probe_kernel_coefficients=probe_kernel_coefficients, cluster_scaling_factor=cluster_scaling_factor, emitted_mapping_matrix=emitted_mapping_matrix, standardize_scaling=standardize_scaling, standardize_offset=standardize_offset, chosen_specialist_ids=chosen_specialist_ids, specialist_mixing_shares=specialist_mixing_shares, specialist_gating_matrices=specialist_gating_matrices, raising_matrices=raising_matrices, lowering_matrices=lowering_matrices)


rms_eps = 1e-06
norm_eps = 1e-05

def causal_conv(series, tap_weights, rim_rows):
    padded = jnp.concatenate([rim_rows, series], axis=0).astype(jnp.float32)
    length = series.shape[0]
    running = jnp.zeros(series.shape, jnp.float32)
    for tap_index in range(tap_weights.shape[0]):
        running = running + tap_weights[tap_index].astype(jnp.float32) * lax.slice_in_dim(padded, tap_index, tap_index + length, axis=0)
    return jax.nn.silu(running).astype(jnp.bfloat16)

def ssd_blocks(x_conv, b_conv, c_conv, increment_delta, fading_exponent, init_state, block_len):
    length, head_count, head_width = x_conv.shape
    state_width = b_conv.shape[2]
    block_count = length // block_len
    x_block = x_conv.reshape(block_count, block_len, head_count, head_width).astype(jnp.float32)
    b_block = b_conv.reshape(block_count, block_len, head_count, state_width).astype(jnp.float32)
    c_block = c_conv.reshape(block_count, block_len, head_count, state_width).astype(jnp.float32)
    cumulative = jnp.cumsum(jnp.transpose(fading_exponent.reshape(block_count, block_len, head_count), (0, 2, 1)), axis=2)
    step_heads = jnp.transpose(increment_delta.reshape(block_count, block_len, head_count), (0, 2, 1))
    causal = jnp.arange(block_len)[:, None] >= jnp.arange(block_len)[None, :]
    within = jnp.exp(jnp.where(causal, cumulative[:, :, :, None] - cumulative[:, :, None, :], -jnp.inf))
    scores = jnp.einsum('cthn,cshn->chts', c_block, b_block)
    mixing = (scores * within * step_heads[:, :, None, :]).astype(jnp.bfloat16)
    diag_out = jnp.einsum('chts,cshp->cthp', mixing.astype(jnp.float32), x_block)
    tail_decay = jnp.exp(cumulative[:, :, -1:] - cumulative) * step_heads
    scaled = (x_block * jnp.transpose(tail_decay, (0, 2, 1))[:, :, :, None]).astype(jnp.bfloat16)
    block_state = jnp.einsum('cshp,cshn->chpn', scaled.astype(jnp.float32), b_block)
    totals = cumulative[:, :, -1]
    through = jnp.cumsum(totals, axis=0)
    before = through - totals
    earlier = jnp.arange(block_count)[:, None] > jnp.arange(block_count)[None, :]
    carry_weight = jnp.exp(jnp.where(earlier[:, :, None], before[:, None, :] - through[None, :, :], -jnp.inf))
    entering = jnp.einsum('cjh,jhpn->chpn', carry_weight, block_state, precision=lax.Precision.HIGHEST) + jnp.exp(before)[:, :, None, None] * init_state[None]
    reach_decay = jnp.transpose(jnp.exp(cumulative), (0, 2, 1))
    carried_out = jnp.einsum('cthn,chpn->cthp', c_block, entering, precision=lax.Precision.HIGHEST) * reach_decay[:, :, :, None]
    outcome = (diag_out + carried_out).reshape(length, head_count, head_width)
    final_state = jnp.einsum('jh,jhpn->hpn', jnp.exp(through[-1][None, :] - through), block_state, precision=lax.Precision.HIGHEST) + jnp.exp(through[-1])[:, None, None] * init_state
    return (outcome, final_state, through[-1])

def reference(skip_connection_stream, emitted_valve_unscaled, channel_source_mapped, hidden_source_mapped, probe_mapped_values, increment_premapped, extra_log_fading, channel_fading_speed, channel_source_kernel, hidden_source_kernel, probe_kernel_coefficients, cluster_scaling_factor, emitted_mapping_matrix, standardize_scaling, standardize_offset, chosen_specialist_ids, specialist_mixing_shares, specialist_gating_matrices, raising_matrices, lowering_matrices):
    per_group = HEADS // GROUPS
    tap_weights = jnp.concatenate([channel_source_kernel, hidden_source_kernel, probe_kernel_coefficients], axis=1)

    def lone_token_list(token_segments):
        channel_source_list, hidden_source_list, probe_value_list, increment_list, extra_fading_list = token_segments
        joined_rows = jnp.concatenate([channel_source_list, hidden_source_list, probe_value_list], axis=1)
        rim_rows = jnp.zeros((KERNEL - 1, joined_rows.shape[1]), jnp.bfloat16)
        convolved = causal_conv(joined_rows, tap_weights, rim_rows)
        x_conv = convolved[:, :INNER].reshape(LEN, HEADS, HEAD_DIM)
        b_conv = jnp.repeat(convolved[:, INNER:INNER + GROUPS * STATE].reshape(LEN, GROUPS, STATE), per_group, axis=1)
        c_conv = jnp.repeat(convolved[:, INNER + GROUPS * STATE:].reshape(LEN, GROUPS, STATE), per_group, axis=1)
        increment_delta = jax.nn.softplus(increment_list)
        fading_exponent = extra_fading_list - channel_fading_speed[None, :] * increment_delta
        init_state = jnp.zeros((HEADS, HEAD_DIM, STATE), jnp.float32)
        outcome, final_state, total_decay = ssd_blocks(x_conv, b_conv, c_conv, increment_delta, fading_exponent, init_state, BLK)
        return outcome.reshape(LEN, INNER).astype(jnp.bfloat16)
    blending_outcome = lax.map(lone_token_list, (channel_source_mapped, hidden_source_mapped, probe_mapped_values, increment_premapped, extra_log_fading))
    all_rows = BATCH * LEN
    gated = blending_outcome.reshape(all_rows, INNER).astype(jnp.float32) * jax.nn.silu(emitted_valve_unscaled.reshape(all_rows, INNER).astype(jnp.float32))
    grouped = gated.reshape(all_rows, GROUPS, INNER // GROUPS)
    grouped = grouped * lax.rsqrt(lax.optimization_barrier(jnp.mean(grouped * grouped, axis=-1, keepdims=True)) + rms_eps)
    group_normed = (grouped.reshape(all_rows, INNER) * cluster_scaling_factor[None, :]).astype(jnp.bfloat16)
    pre_norm = skip_connection_stream.reshape(all_rows, D).astype(jnp.float32) + jnp.dot(group_normed, emitted_mapping_matrix, preferred_element_type=jnp.float32)
    centre = lax.optimization_barrier(jnp.mean(pre_norm, axis=-1, keepdims=True))
    variance = lax.optimization_barrier(jnp.mean(jnp.square(pre_norm - centre), axis=-1, keepdims=True))
    normed = ((pre_norm - centre) * lax.rsqrt(variance + norm_eps) * standardize_scaling[None, :] + standardize_offset[None, :]).astype(jnp.bfloat16)
    flat_ids = chosen_specialist_ids.reshape(-1).astype(jnp.int32)
    flat_weights = specialist_mixing_shares.reshape(-1).astype(jnp.float32)
    owner = (jnp.arange(all_rows * 2, dtype=jnp.int32) // 2).astype(jnp.int32)
    buffer_rows = N_SP * N_DP * CAP
    padded_rows = jnp.concatenate([normed, jnp.zeros((1, D), jnp.bfloat16)], axis=0)

    def one_expert(running, expert):
        matched = flat_ids == expert
        ranked = jnp.cumsum(matched.astype(jnp.int32)) - 1
        placed = jnp.where(matched, ranked, buffer_rows).astype(jnp.int32)
        source = jnp.full((buffer_rows + 1,), all_rows, jnp.int32).at[placed].set(owner)[:buffer_rows]
        weight_at = jnp.zeros((buffer_rows + 1,), jnp.float32).at[placed].set(flat_weights)[:buffer_rows]
        rows_in = padded_rows[source]
        gate_val = jnp.dot(rows_in, specialist_gating_matrices[expert], preferred_element_type=jnp.float32)
        up_val = jnp.dot(rows_in, raising_matrices[expert], preferred_element_type=jnp.float32)
        hidden = (jax.nn.silu(gate_val) * up_val).astype(jnp.bfloat16)
        expert_sum = jnp.zeros((buffer_rows, D), jnp.float32)
        for part_index in range(N_DP):
            lower = part_index * FF_PART
            partial_value = jnp.dot(hidden[:, lower:lower + FF_PART], lowering_matrices[expert, lower:lower + FF_PART], preferred_element_type=jnp.float32).astype(jnp.bfloat16)
            expert_sum = expert_sum + lax.optimization_barrier(partial_value).astype(jnp.float32)
        expert_out = expert_sum.astype(jnp.bfloat16)
        running = running.at[source].add(weight_at[:, None] * expert_out.astype(jnp.float32))
        return (running, None)
    routed_sum, unused = lax.scan(one_expert, jnp.zeros((all_rows + 1, D), jnp.float32), jnp.arange(EXPERTS, dtype=jnp.int32))
    layer_out = (normed.astype(jnp.float32) + routed_sum[:all_rows]).astype(jnp.bfloat16)
    return layer_out.reshape(BATCH, LEN, D)
```

```python
import jax
import jax.numpy as jnp
from jax import lax
from jax.experimental import pallas as pl
from jax.experimental.pallas import tpu as pltpu
from jax.sharding import PartitionSpec as P


HEADS = 16
HEAD_DIM = 64
GROUPS = 4
STATE = 64
KERNEL = 4
BLK = 128
CHUNKS = 2


rms_eps = 1e-06
norm_eps = 1e-05


def causal_conv(series, tap_weights, rim_rows):
    padded = jnp.concatenate([rim_rows, series], axis=0).astype(jnp.float32)
    length = series.shape[0]
    running = jnp.zeros(series.shape, jnp.float32)
    for tap_index in range(tap_weights.shape[0]):
        running = running + tap_weights[tap_index] * lax.slice_in_dim(
            padded, tap_index, tap_index + length, axis=0
        )
    return jax.nn.silu(running).astype(jnp.bfloat16)


def ssd_blocks(x_conv, b_conv, c_conv, increment_delta, fading_exponent, block_len):
    length, head_count, head_width = x_conv.shape
    state_width = b_conv.shape[2]
    block_count = length // block_len
    x_block = x_conv.reshape(block_count, block_len, head_count, head_width)
    b_block = b_conv.reshape(block_count, block_len, head_count, state_width)
    c_block = c_conv.reshape(block_count, block_len, head_count, state_width)
    cumulative = jnp.cumsum(
        jnp.transpose(fading_exponent.reshape(block_count, block_len, head_count), (0, 2, 1)),
        axis=2,
    )
    step_heads = jnp.transpose(
        increment_delta.reshape(block_count, block_len, head_count), (0, 2, 1)
    )
    causal = jnp.arange(block_len)[:, None] >= jnp.arange(block_len)[None, :]
    within = jnp.exp(
        jnp.where(causal, cumulative[:, :, :, None] - cumulative[:, :, None, :], -jnp.inf)
    )
    scores = jnp.einsum("cthn,cshn->chts", c_block, b_block, preferred_element_type=jnp.float32)
    mixing = (scores * within * step_heads[:, :, None, :]).astype(jnp.bfloat16)
    diag_out = jnp.einsum("chts,cshp->cthp", mixing, x_block, preferred_element_type=jnp.float32)
    tail_decay = jnp.exp(cumulative[:, :, -1:] - cumulative) * step_heads
    scaled = (
        x_block.astype(jnp.float32) * jnp.transpose(tail_decay, (0, 2, 1))[:, :, :, None]
    ).astype(jnp.bfloat16)
    block_state = jnp.einsum("cshp,cshn->chpn", scaled, b_block, preferred_element_type=jnp.float32)
    totals = cumulative[:, :, -1]
    through = jnp.cumsum(totals, axis=0)
    before = through - totals
    earlier = jnp.arange(block_count)[:, None] > jnp.arange(block_count)[None, :]
    carry_weight = jnp.exp(
        jnp.where(earlier[:, :, None], before[:, None, :] - through[None, :, :], -jnp.inf)
    )
    entering = jnp.einsum(
        "cjh,jhpn->chpn", carry_weight, block_state, precision=lax.Precision.HIGHEST
    )
    reach_decay = jnp.transpose(jnp.exp(cumulative), (0, 2, 1))
    carried_out = (
        jnp.einsum(
            "cthn,chpn->cthp",
            c_block.astype(jnp.float32),
            entering,
            precision=lax.Precision.HIGHEST,
        )
        * reach_decay[:, :, :, None]
    )
    return (diag_out + carried_out).reshape(length, head_count, head_width)


def join_kernel(*refs):
    *block_refs, out_ref, sems = refs
    count = block_refs[0].shape[0]
    moves = [
        pltpu.make_async_copy(block, out_ref.at[pl.ds(place * count, count)], sems.at[place])
        for place, block in enumerate(block_refs)
    ]
    for move in moves:
        move.start()
    for move in moves:
        move.wait()


def join_rows(blocks):
    count, width = blocks[0].shape
    if count % 8:
        return jnp.concatenate(blocks, axis=0)
    return pl.pallas_call(
        join_kernel,
        in_specs=[pl.BlockSpec(memory_space=pl.ANY)] * len(blocks),
        out_specs=pl.BlockSpec(memory_space=pltpu.HBM),
        out_shape=jax.ShapeDtypeStruct((count * len(blocks), width), blocks[0].dtype),
        scratch_shapes=[pltpu.SemaphoreType.DMA((len(blocks),))],
        compiler_params=pltpu.CompilerParams(vmem_limit_bytes=1024 * 1024),
        name="join_rows",
    )(*blocks)


def ffn_kernel(*refs):
    count = (len(refs) - 10) // 2
    pieces, (gate_hbm, up_hbm, down_hbm) = refs[:count], refs[count : count + 3]
    outs = refs[count + 3 : 2 * count + 3]
    rows, gate_ref, up_ref, down_ref, hidden_ref, stage, sems = refs[2 * count + 3 :]
    size = pieces[0].shape[0]
    width = rows.shape[1]
    part = hidden_ref.shape[1]
    out_tile = stage.shape[2]
    tile = 256 if part % 256 == 0 else 128
    first = part // tile
    second = width // out_tile

    def columns(place, extent):
        return pl.ds(pl.multiple_of(place * extent, extent), extent)

    def bring_piece(place):
        spot = pl.ds(place * size, size)
        return pltpu.make_async_copy(pieces[place], rows.at[spot], sems.at[0, place])

    def bring_wide(place):
        spot = columns(place, tile)
        return (
            pltpu.make_async_copy(gate_hbm.at[0, :, spot], gate_ref.at[:, spot], sems.at[1, place]),
            pltpu.make_async_copy(up_hbm.at[0, :, spot], up_ref.at[:, spot], sems.at[2, place]),
        )

    def bring_down(place):
        spot = columns(place, out_tile)
        return pltpu.make_async_copy(
            down_hbm.at[0, :, spot], down_ref.at[:, spot], sems.at[3, place]
        )

    def send(place, which):
        return [
            pltpu.make_async_copy(
                stage.at[which, pl.ds(spot * size, size)],
                out.at[:, columns(place, out_tile)],
                sems.at[4 + which, spot],
            )
            for spot, out in enumerate(outs)
        ]

    def widen(block, place):
        spot = columns(place, tile)
        gate_val = jnp.dot(block, gate_ref[:, spot], preferred_element_type=jnp.float32)
        up_val = jnp.dot(block, up_ref[:, spot], preferred_element_type=jnp.float32)
        return (gate_val * jax.nn.sigmoid(gate_val) * up_val).astype(jnp.bfloat16)

    for move in bring_wide(0):
        move.start()
    for place in range(count):
        bring_piece(place).start()
    for place in range(1, first):
        for move in bring_wide(place):
            move.start()
    for place in range(second):
        bring_down(place).start()

    for move in bring_wide(0):
        move.wait()
    for place in range(count):
        bring_piece(place).wait()
        spot = pl.ds(place * size, size)
        hidden_ref[spot, pl.ds(0, tile)] = widen(rows[spot, :], 0)

    def wide_step(place, carry):
        for move in bring_wide(place):
            move.wait()
        hidden_ref[:, columns(place, tile)] = widen(rows[...], place)
        return carry

    lax.fori_loop(1, first, wide_step, 0)

    def down_step(place, carry):
        which = lax.rem(place, 2)
        bring_down(place).wait()
        partial = jnp.dot(
            hidden_ref[...], down_ref[:, columns(place, out_tile)], preferred_element_type=jnp.float32
        )

        @pl.when(place >= 2)
        def _():
            for move in send(place - 2, which):
                move.wait()

        stage[which] = partial.astype(jnp.bfloat16)
        for move in send(place, which):
            move.start()
        return carry

    lax.fori_loop(0, second, down_step, 0)
    for place in range(max(second - 2, 0), second):
        for move in send(place, place % 2):
            move.wait()


def expert_part(pieces, gate_w, up_w, down_w):
    count, width = pieces[0].shape
    total = count * len(pieces)
    part = gate_w.shape[2]
    out_tile = 512
    hbm = pl.BlockSpec(memory_space=pltpu.HBM)
    return pl.pallas_call(
        ffn_kernel,
        in_specs=[hbm] * (len(pieces) + 3),
        out_specs=[hbm] * len(pieces),
        out_shape=[jax.ShapeDtypeStruct((count, width), jnp.bfloat16)] * len(pieces),
        scratch_shapes=[
            pltpu.VMEM((total, width), jnp.bfloat16),
            pltpu.VMEM((width, part), jnp.bfloat16),
            pltpu.VMEM((width, part), jnp.bfloat16),
            pltpu.VMEM((part, width), jnp.bfloat16),
            pltpu.VMEM((total, part), jnp.bfloat16),
            pltpu.VMEM((2, total, out_tile), jnp.bfloat16),
            pltpu.SemaphoreType.DMA((6, max(len(pieces), part // 128, width // out_tile))),
        ],
        compiler_params=pltpu.CompilerParams(vmem_limit_bytes=36 * 1024 * 1024),
        cost_estimate=pl.CostEstimate(
            flops=total * width * part * 6,
            transcendentals=total * part,
            bytes_accessed=3 * width * part * 2 + 4 * total * width,
        ),
        name="expert_part",
    )(*[pltpu.with_memory_space_constraint(v, pltpu.HBM) for v in (*pieces, gate_w, up_w, down_w)])


def flip(value, mask):
    size = lax.axis_size("dp")
    return lax.ppermute(value, "dp", [(i, i ^ mask) for i in range(size)])


def exchange(blocks):
    size = lax.axis_size("sp")
    arrived = [blocks[0]]
    for gap in range(1, size):
        arrived.append(lax.ppermute(blocks[gap], "sp", [(i, i ^ gap) for i in range(size)]))
    return arrived


def routed(normed, ids, shares, gate_w, up_w, down_w):
    sp_size = lax.axis_size("sp")
    dp_size = lax.axis_size("dp")
    tok_rows, width = normed.shape
    slot_cap = 3 * tok_rows // sp_size
    flat_ids = ids.reshape(-1)
    matched = (flat_ids[:, None] == jnp.arange(sp_size, dtype=jnp.int32)[None, :]).astype(jnp.int32)
    ranked = jnp.cumsum(matched, axis=0) - 1
    rank = jnp.sum(matched * ranked, axis=1).reshape(tok_rows, 2)
    gaps = ids ^ lax.axis_index("sp").astype(jnp.int32)
    span = slot_cap // CHUNKS
    total = normed.astype(jnp.float32)
    parts = []
    for chunk in range(CHUNKS):
        local = rank - chunk * span
        inside = (local >= 0) & (local < span)
        place = jnp.where(inside, gaps * span + local, -1)
        slots = jnp.arange(sp_size * span, dtype=jnp.int32)
        hit = slots[:, None, None] == place[None, :, :]
        placing = jnp.sum(hit.astype(jnp.bfloat16), axis=2)
        outgoing = (
            jnp.dot(placing, normed, preferred_element_type=jnp.float32)
            .astype(jnp.bfloat16)
            .reshape(sp_size, span, width)
        )
        weight = jnp.sum(
            jnp.where(place[:, :, None] == slots[None, None, :], shares[:, :, None], 0.0), axis=1
        )
        high = weight.astype(jnp.bfloat16)
        low = (weight - high.astype(jnp.float32)).astype(jnp.bfloat16)
        own = join_rows(exchange(outgoing))
        parts.append((own, jnp.concatenate([high, low], axis=0)))
    masks = [1 << bit for bit in range(1, dp_size.bit_length() - 1)] + [1]
    for own, spread in parts:
        pieces = [own]
        for mask in masks:
            pieces = pieces + [flip(piece, mask) for piece in pieces]
        sums = [[value] for value in expert_part(pieces, gate_w, up_w, down_w)]
        for mask in masks[::-1]:
            half = len(sums) // 2
            for place in range(half - 1, -1, -1):
                leaving = sums[half + place]
                sent = leaving[0]
                if len(leaving) > 1:
                    sent = sum(v.astype(jnp.float32) for v in leaving).astype(jnp.bfloat16)
                sums[place].append(flip(sent, mask))
            sums = sums[:half]
        mine = sum(v.astype(jnp.float32) for v in sums[0]).astype(jnp.bfloat16)
        answer = jnp.concatenate(exchange(mine.reshape(sp_size, span, width)), axis=0)
        both = jnp.dot(spread, answer, preferred_element_type=jnp.float32)
        total = total + both[:tok_rows] + both[tok_rows:]
    return total.astype(jnp.bfloat16)


def per_device(
    skip_connection_stream,
    emitted_valve_unscaled,
    channel_source_mapped,
    hidden_source_mapped,
    probe_mapped_values,
    increment_premapped,
    extra_log_fading,
    channel_fading_speed,
    channel_source_kernel,
    hidden_source_kernel,
    probe_kernel_coefficients,
    cluster_scaling_factor,
    emitted_mapping_matrix,
    standardize_scaling,
    standardize_offset,
    chosen_specialist_ids,
    specialist_mixing_shares,
    specialist_gating_matrices,
    raising_matrices,
    lowering_matrices,
):
    sp_size = lax.axis_size("sp")
    sp_index = lax.axis_index("sp")
    tok_rows = skip_connection_stream.shape[1]
    inner_width = HEADS * HEAD_DIM
    per_group = HEADS // GROUPS
    paired = HEAD_DIM + 2 * STATE
    head_count = HEADS // sp_size
    first_head = sp_index * head_count
    x_heads = channel_source_mapped[0].reshape(tok_rows, HEADS, HEAD_DIM)
    b_heads = jnp.repeat(
        hidden_source_mapped[0].reshape(tok_rows, GROUPS, STATE), per_group, axis=1
    )
    c_heads = jnp.repeat(probe_mapped_values[0].reshape(tok_rows, GROUPS, STATE), per_group, axis=1)
    payload = jnp.concatenate([x_heads, b_heads, c_heads], axis=2)
    arrived = lax.all_to_all(payload, "sp", split_axis=1, concat_axis=0, tiled=True)
    taps_x = lax.dynamic_slice_in_dim(
        channel_source_kernel.reshape(KERNEL, HEADS, HEAD_DIM), first_head, head_count, 1
    )
    taps_b = lax.dynamic_slice_in_dim(
        jnp.repeat(hidden_source_kernel.reshape(KERNEL, GROUPS, STATE), per_group, axis=1),
        first_head,
        head_count,
        1,
    )
    taps_c = lax.dynamic_slice_in_dim(
        jnp.repeat(probe_kernel_coefficients.reshape(KERNEL, GROUPS, STATE), per_group, axis=1),
        first_head,
        head_count,
        1,
    )
    rim_rows = jnp.zeros((KERNEL - 1, head_count, paired), jnp.bfloat16)
    convolved = causal_conv(arrived, jnp.concatenate([taps_x, taps_b, taps_c], axis=2), rim_rows)
    increment_delta = jax.nn.softplus(increment_premapped[0])
    speeds_per_channel = lax.dynamic_slice_in_dim(channel_fading_speed, first_head, head_count, 0)
    fading_exponent = extra_log_fading[0] - speeds_per_channel[None, :] * increment_delta
    outcome = ssd_blocks(
        convolved[:, :, :HEAD_DIM],
        convolved[:, :, HEAD_DIM : HEAD_DIM + STATE],
        convolved[:, :, HEAD_DIM + STATE :],
        increment_delta,
        fading_exponent,
        BLK,
    )
    returned_rows = lax.all_to_all(
        outcome.astype(jnp.bfloat16), "sp", split_axis=0, concat_axis=1, tiled=True
    )
    blending_outcome = returned_rows.reshape(tok_rows, inner_width)
    gated = blending_outcome.astype(jnp.float32) * jax.nn.silu(
        emitted_valve_unscaled[0].astype(jnp.float32)
    )
    grouped = gated.reshape(tok_rows, GROUPS, inner_width // GROUPS)
    grouped = grouped * lax.rsqrt(jnp.mean(grouped * grouped, axis=-1, keepdims=True) + rms_eps)
    group_normed = (
        grouped.reshape(tok_rows, inner_width) * cluster_scaling_factor[None, :]
    ).astype(jnp.bfloat16)
    pre_norm = skip_connection_stream[0].astype(jnp.float32) + jnp.dot(
        group_normed, emitted_mapping_matrix, preferred_element_type=jnp.float32
    )
    centre = jnp.mean(pre_norm, axis=-1, keepdims=True)
    variance = jnp.mean(jnp.square(pre_norm - centre), axis=-1, keepdims=True)
    normed = (
        (pre_norm - centre) * lax.rsqrt(variance + norm_eps) * standardize_scaling[None, :]
        + standardize_offset[None, :]
    ).astype(jnp.bfloat16)
    layer_out = routed(
        normed,
        chosen_specialist_ids[0],
        specialist_mixing_shares[0],
        specialist_gating_matrices,
        raising_matrices,
        lowering_matrices,
    )
    return layer_out[None]


def solution(mesh):
    placed = (
        P("dp", "sp", None),
        P("dp", "sp", None),
        P("dp", "sp", None),
        P("dp", "sp", None),
        P("dp", "sp", None),
        P("dp", None, "sp"),
        P("dp", None, "sp"),
        P(),
        P(),
        P(),
        P(),
        P(),
        P(),
        P(),
        P(),
        P("dp", "sp", None),
        P("dp", "sp", None),
        P("sp", None, "dp"),
        P("sp", None, "dp"),
        P("sp", "dp", None),
    )
    return jax.shard_map(
        per_device, mesh=mesh, in_specs=placed, out_specs=P("dp", "sp", None), check_vma=False
    )
```
